32 devices in a mesh: rep: 2 (over x), fs: 8 (over z, y), tp: 2 (over core).
Axes of the slice: x: 2, y: 2, z: 4, core: 2. Of those that a mesh axis runs over, the one named last changes fastest.
Arguments:
- tokens: bfloat16 [8192, 2048], P(('rep', 'fs')), may hold values from -6 to 6
- mix_gain: bfloat16 [2048], replicated, may hold values from 0.099609375 to 1.8984375
- value_weight: bfloat16 [2048, 1536], P('fs', 'tp'), may hold values from -0.125 to 0.125
- outer_gate_weight: bfloat16 [2048, 1536], P('fs', 'tp'), may hold values from -0.125 to 0.125
- inner_gate_weight: bfloat16 [2048, 1536], P('fs', 'tp'), may hold values from -0.125 to 0.125
- conv_taps: bfloat16 [3, 1536], P(None, 'tp'), may hold values from -3 to 3
- mix_out_weight: bfloat16 [1536, 2048], P('tp', 'fs'), may hold values from -0.15625 to 0.15625
- ffn_gain: bfloat16 [2048], replicated, may hold values from 0.099609375 to 1.8984375
- gate_weight: bfloat16 [2048, 4096], P('fs', 'tp'), may hold values from -0.125 to 0.125
- up_weight: bfloat16 [2048, 4096], P('fs', 'tp'), may hold values from -0.125 to 0.125
- down_weight: bfloat16 [4096, 2048], P('tp', 'fs'), may hold values from -0.09375 to 0.09375
Outputs:
- layer_out: bfloat16 [8192, 2048], P(('rep', 'fs'))
The draws below stay inside these ranges and needn't reach their ends.
All inputs are finite; a program needn't handle non-finite values.
Results may differ from the reference program's by a relative error of at most 0.02.
Values may be sent and summed in bfloat16 or wider, within the bound.
No kernel may reach another device: no remote copies, remote signals or barrier semaphores. Data moves between devices by JAX's collectives and lax.ppermute only.
A program may use at most 128 MiB of HBM per device.

```python
import jax
import jax.numpy as jnp
from jax import lax

D = 2048
C = 1536
FF = 4096
TAPS = 3
SEQ_GRP = 2
ROWS = 512
TOKENS = 8192
N_TP = 2


def levels(own_key, extent, pieces, least, largest):
    level = 1.0
    for dim, parts in pieces:
        draws = jax.random.uniform(jax.random.fold_in(jax.random.fold_in(own_key, 6), dim), (parts,), jnp.float32, least / len(pieces), largest / len(pieces))
        level = level * jnp.repeat(jnp.exp(draws), extent[dim] // parts).reshape((-1,) + (1,) * (len(extent) - 1 - dim))
    return level


def gaussian(key, shape, spread, limit, shards=(), held_as=jnp.bfloat16):
    level = levels(key, shape, shards, -0.22, 0.18) if shards else 1.0
    entries = jax.random.normal(key, shape, jnp.float32) * spread * level
    return jnp.minimum(jnp.maximum(entries, -limit), limit).astype(held_as)


def setup_inputs(seed: int = 0) -> dict:
    splits = jax.random.split(jax.random.key(seed), 12)
    return {
        "tokens": gaussian(splits[0], (TOKENS, D), 1.0, 6.0, ((0, 16),)),
        "mix_gain": jnp.clip(1.0 + 0.18 * jax.random.normal(splits[1], (D,), jnp.float32), 0.099609375, 1.8984375).astype(jnp.bfloat16),
        "value_weight": gaussian(splits[2], (D, C), D ** -0.5, 0.125, ((0, 8), (1, 2))),
        "outer_gate_weight": gaussian(splits[3], (D, C), D ** -0.5, 0.125, ((0, 8), (1, 2))),
        "inner_gate_weight": gaussian(splits[4], (D, C), D ** -0.5, 0.125, ((0, 8), (1, 2))),
        "conv_taps": gaussian(splits[5], (TAPS, C), 0.58, 3.0, ((1, 2),)),
        "mix_out_weight": gaussian(splits[6], (C, D), C ** -0.5, 0.15625, ((0, 2), (1, 8))),
        "ffn_gain": jnp.clip(1.0 + 0.18 * jax.random.normal(splits[7], (D,), jnp.float32), 0.099609375, 1.8984375).astype(jnp.bfloat16),
        "gate_weight": gaussian(splits[8], (D, FF), D ** -0.5, 0.125, ((0, 8), (1, 2))),
        "up_weight": gaussian(splits[9], (D, FF), D ** -0.5, 0.125, ((0, 8), (1, 2))),
        "down_weight": gaussian(splits[10], (FF, D), FF ** -0.5, 0.09375, ((0, 2), (1, 8))),
    }


EPS = 1e-05

def rms_norm(values, gain):
    floats = values.astype(jnp.float32)
    scaled = floats * lax.rsqrt(lax.optimization_barrier(jnp.mean(floats * floats, axis=-1, keepdims=True)) + EPS)
    return (scaled * gain.astype(jnp.float32)).astype(jnp.bfloat16)

def short_conv(value_proj, outer_proj, inner_proj, conv_taps, seq_len):
    mixed_in = inner_proj.astype(jnp.float32) * value_proj.astype(jnp.float32)
    count_rows = mixed_in.shape[0]
    position = (jnp.arange(count_rows, dtype=jnp.int32) % seq_len)[:, None]
    zero_row = jnp.zeros((1, mixed_in.shape[1]), jnp.float32)
    back_one = jnp.where(position >= 1, jnp.concatenate([zero_row, mixed_in[:-1]], axis=0), 0.0)
    back_two = jnp.where(position >= 2, jnp.concatenate([zero_row, zero_row, mixed_in[:-2]], axis=0), 0.0)
    taps = conv_taps.astype(jnp.float32)
    convolved = taps[0] * back_two + taps[1] * back_one + taps[2] * mixed_in
    return (outer_proj.astype(jnp.float32) * convolved).astype(jnp.bfloat16)

def split_sum(left, right, groups):
    group_cols = left.shape[1] // groups
    summed = jnp.zeros((left.shape[0], right.shape[1]), jnp.float32)
    for shard_number in range(groups):
        low = shard_number * group_cols
        partial_value = jnp.dot(left[:, low:low + group_cols], right[low:low + group_cols], preferred_element_type=jnp.float32).astype(jnp.bfloat16)
        partial_value = lax.optimization_barrier(partial_value)
        summed = summed + partial_value.astype(jnp.float32)
    return summed

def reference(tokens, mix_gain, value_weight, outer_gate_weight, inner_gate_weight, conv_taps, mix_out_weight, ffn_gain, gate_weight, up_weight, down_weight):
    seq_len = ROWS // SEQ_GRP
    normed = rms_norm(tokens, mix_gain)
    value_proj = jnp.dot(normed, value_weight, preferred_element_type=jnp.float32).astype(jnp.bfloat16)
    outer_proj = jnp.dot(normed, outer_gate_weight, preferred_element_type=jnp.float32).astype(jnp.bfloat16)
    inner_proj = jnp.dot(normed, inner_gate_weight, preferred_element_type=jnp.float32).astype(jnp.bfloat16)
    mixed = short_conv(value_proj, outer_proj, inner_proj, conv_taps, seq_len)
    after_mix = (tokens.astype(jnp.float32) + split_sum(mixed, mix_out_weight, N_TP)).astype(jnp.bfloat16)
    normed_two = rms_norm(after_mix, ffn_gain)
    gate_proj = jnp.dot(normed_two, gate_weight, preferred_element_type=jnp.float32)
    up_proj = jnp.dot(normed_two, up_weight, preferred_element_type=jnp.float32)
    hidden = (jax.nn.silu(gate_proj) * up_proj).astype(jnp.bfloat16)
    return (after_mix.astype(jnp.float32) + split_sum(hidden, down_weight, N_TP)).astype(jnp.bfloat16)
```

```python
import jax
import jax.numpy as jnp
from jax import lax
from jax.sharding import PartitionSpec as P

SEQ_GRP = 2


EPS = 1e-05


def scaled_rows(floats, gain):
    scaled = floats * lax.rsqrt(jnp.mean(floats * floats, axis=-1, keepdims=True) + EPS)
    return (scaled * gain.astype(jnp.float32)).astype(jnp.bfloat16)


def short_conv(value_proj, outer_proj, inner_proj, conv_taps, seq_len):
    mixed_in = inner_proj.astype(jnp.float32) * value_proj.astype(jnp.float32)
    count_rows = mixed_in.shape[0]
    position = (jnp.arange(count_rows, dtype=jnp.int32) % seq_len)[:, None]
    zero_row = jnp.zeros((1, mixed_in.shape[1]), jnp.float32)
    back_one = jnp.where(position >= 1, jnp.concatenate([zero_row, mixed_in[:-1]], axis=0), 0.0)
    back_two = jnp.where(
        position >= 2, jnp.concatenate([zero_row, zero_row, mixed_in[:-2]], axis=0), 0.0
    )
    taps = conv_taps.astype(jnp.float32)
    convolved = taps[0] * back_two + taps[1] * back_one + taps[2] * mixed_in
    return (outer_proj.astype(jnp.float32) * convolved).astype(jnp.bfloat16)


def shift(values, axis, by):
    size = lax.axis_size(axis)
    return lax.ppermute(values, axis, [(i, (i + by) % size) for i in range(size)])


def ring_order(size):
    return list(range(0, size, 2)) + [i for i in range(size - 1, 0, -1) if i % 2]


def slot_offsets(size):
    offsets = [0]
    for hop in range(1, (size - 1) // 2 + 1):
        offsets += [-hop, hop]
    if size % 2 == 0 and size > 1:
        offsets.append(size // 2)
    return offsets


def ring_gather(shard):
    size = lax.axis_size("fs")
    ring = ring_order(size)
    ahead = [(ring[i], ring[(i + 1) % size]) for i in range(size)]
    behind = [(to, source) for source, to in ahead]
    slots = [shard]
    up, down = shard, shard
    for _ in range((size - 1) // 2):
        up = lax.ppermute(up, "fs", ahead)
        down = lax.ppermute(down, "fs", behind)
        slots += [up, down]
    if size % 2 == 0 and size > 1:
        half = shard.shape[0] // 2
        first = lax.ppermute(up[:half], "fs", ahead)
        second = lax.ppermute(down[half:], "fs", behind)
        slots.append(jnp.concatenate([first, second], axis=0))
    return slots


def slot_sources():
    size = lax.axis_size("fs")
    ring = ring_order(size)
    place = [0] * size
    for where, member in enumerate(ring):
        place[member] = where
    table = jnp.array(
        [[ring[(place[m] + o) % size] for o in slot_offsets(size)] for m in range(size)], jnp.int32
    )
    row = lax.dynamic_index_in_dim(table, lax.axis_index("fs"), 0, keepdims=False)
    return [row[slot] for slot in range(size)]


def pick_columns(values, sources, width):
    return jnp.concatenate(
        [lax.dynamic_slice_in_dim(values, s * width, width, values.ndim - 1) for s in sources],
        axis=-1,
    )


def reduce_groups(blocks):
    sums = []
    for row in blocks:
        total = row[0].astype(jnp.float32)
        for j in range(1, len(row)):
            total = total + shift(row[j], "tp", j).astype(jnp.float32)
        sums.append(total)
    total = sums[0]
    for i in range(1, len(sums)):
        total = total + shift(sums[i].astype(jnp.bfloat16), "rep", i).astype(jnp.float32)
    return total


def local(
    tokens,
    mix_gain,
    value_weight,
    outer_gate_weight,
    inner_gate_weight,
    conv_taps,
    mix_out_weight,
    ffn_gain,
    gate_weight,
    up_weight,
    down_weight,
):
    reps, tps, members = lax.axis_size("rep"), lax.axis_size("tp"), lax.axis_size("fs")
    rep, tp = lax.axis_index("rep"), lax.axis_index("tp")
    row_count, model = tokens.shape
    share = row_count // tps
    seq_len = row_count // SEQ_GRP
    width = model // members

    def own(weight, axis):
        part = weight.shape[axis] // reps
        return lax.dynamic_slice_in_dim(weight, rep * part, part, axis)

    mix_in = jnp.concatenate(
        [own(value_weight, 1), own(inner_gate_weight, 1), own(outer_gate_weight, 1)], axis=1
    )
    chans = mix_in.shape[1] // 3
    in_slots = ring_gather(mix_in)
    out_slots = ring_gather(own(mix_out_weight, 0))
    gate_slots = ring_gather(own(gate_weight, 1))
    up_slots = ring_gather(own(up_weight, 1))
    down_slots = ring_gather(own(down_weight, 0))
    taps = own(conv_taps, 1)

    sources = slot_sources()
    turned = pick_columns(tokens, sources, width)
    gain_one = pick_columns(mix_gain, sources, width)
    gain_two = pick_columns(ffn_gain, sources, width)

    groups = [turned] + [
        shift(turned, "rep", -i) for i in range(1, reps)
    ]
    normed = jnp.concatenate(
        [scaled_rows(g.astype(jnp.float32), gain_one) for g in groups], axis=0
    )
    projected = jnp.dot(
        normed, jnp.concatenate(in_slots, axis=0), preferred_element_type=jnp.float32
    ).astype(jnp.bfloat16)
    mixed = short_conv(
        projected[:, :chans],
        projected[:, 2 * chans :],
        projected[:, chans : 2 * chans],
        taps,
        seq_len,
    )
    partial = jnp.dot(
        mixed, jnp.concatenate(out_slots, axis=1), preferred_element_type=jnp.float32
    ).astype(jnp.bfloat16)
    blocks = [
        [
            lax.dynamic_slice_in_dim(
                partial, i * row_count + ((tp + j) % tps) * share, share, 0
            )
            for j in range(tps)
        ]
        for i in range(reps)
    ]
    own_rows = lax.dynamic_slice_in_dim(turned, tp * share, share, 0).astype(jnp.float32)
    after_mix = (own_rows + reduce_groups(blocks)).astype(jnp.bfloat16)
    kept = after_mix.astype(jnp.float32)
    normed_two = scaled_rows(kept, gain_two)

    across = [normed_two] + [shift(normed_two, "rep", -i) for i in range(1, reps)]
    rows_two = []
    for piece in across:
        rows_two += [piece] + [shift(piece, "tp", -j) for j in range(1, tps)]
    rows_two = jnp.concatenate(rows_two, axis=0)
    gate_proj = jnp.dot(
        rows_two, jnp.concatenate(gate_slots, axis=0), preferred_element_type=jnp.float32
    )
    up_proj = jnp.dot(
        rows_two, jnp.concatenate(up_slots, axis=0), preferred_element_type=jnp.float32
    )
    hidden = (jax.nn.silu(gate_proj) * up_proj).astype(jnp.bfloat16)

    finished = []
    for low, high in ((0, 3), (3, 5), (5, members)) if members > 5 else ((0, members),):
        weight = jnp.concatenate(down_slots[low:high], axis=1)
        part = jnp.dot(hidden, weight, preferred_element_type=jnp.float32).astype(jnp.bfloat16)
        part = part.reshape(reps, tps, share, -1)
        total = reduce_groups([[part[i, j] for j in range(tps)] for i in range(reps)])
        done = (kept[:, low * width : high * width] + total).astype(jnp.bfloat16)
        pieces = [done] + [shift(done, "tp", -j) for j in range(1, tps)]
        finished.append(pieces)
    out = jnp.zeros((row_count, model), jnp.bfloat16)
    for j in range(tps):
        whole = jnp.concatenate([pieces[j] for pieces in finished], axis=1)
        for slot, source in enumerate(sources):
            out = lax.dynamic_update_slice(
                out,
                whole[:, slot * width : (slot + 1) * width],
                (((tp + j) % tps) * share, source * width),
            )
    return out


def solution(mesh):
    placed = (
        P(("rep", "fs"), None),
        P(),
        P("fs", "tp"),
        P("fs", "tp"),
        P("fs", "tp"),
        P(None, "tp"),
        P("tp", "fs"),
        P(),
        P("fs", "tp"),
        P("fs", "tp"),
        P("tp", "fs"),
    )
    return jax.shard_map(
        local, mesh=mesh, in_specs=placed, out_specs=P(("rep", "fs"), None), check_vma=False
    )
```
